32 devices in a mesh: kv: 8 (over z, x), tp: 4 (over y, core).
Axes of the slice: x: 2, y: 2, z: 4, core: 2. Of those that a mesh axis runs over, the one named last changes fastest.
Arguments:
- tokens: bfloat16 [16, 4096], P(None, 'kv'), may hold values from -400 to 400
- norm_gain: bfloat16 [4096], P('kv'), may hold values from 0.099609375 to 1.8984375
- query_weight: bfloat16 [4096, 4096], P('kv', 'tp'), may hold values from -0.09375 to 0.09375
- key_weight: bfloat16 [4096, 4096], P('kv', 'tp'), may hold values from -0.5 to 0.5
- value_weight: bfloat16 [4096, 4096], P('kv', 'tp'), may hold values from -0.09375 to 0.09375
- out_weight: bfloat16 [4096, 4096], P('tp', 'kv'), may hold values from -0.09375 to 0.09375
- diff_scale: float32 [32], P('tp'), may hold values from 0.3 to 0.8
- head_gain: float32 [128], replicated, may hold values from 0.1 to 1.9
- key_cache: bfloat16 [1, 1024, 32, 128], P(None, 'kv', 'tp'), may hold values from -96 to 96
- value_cache: bfloat16 [1, 1024, 32, 128], P(None, 'kv', 'tp'), may hold values from -6 to 6
- cache_filled: int32 [1], replicated, may hold values from 512 to 992
- accepted: int32 [1], replicated, may hold values from 0 to 16
- parents: int32 [1, 16], replicated, may hold values from -1 to 14, as said below
Outputs:
- mixed: bfloat16 [16, 4096], P(None, 'kv')
- key_cache_new: bfloat16 [1, 1024, 32, 128], P(None, 'kv', 'tp')
- value_cache_new: bfloat16 [1, 1024, 32, 128], P(None, 'kv', 'tp')
The draws below stay inside these ranges and needn't reach their ends.
Inputs may be any that keep to these rules, and one draw needn't show every extreme that they name: `parents`: the parent of proposal j is -1 or an earlier proposal of the same sequence; proposal 0's parent is -1; the last proposal's parent is the proposal before it.
All inputs are finite; a program needn't handle non-finite values.
Results may differ from the reference program's by a relative error of at most 0.015.
Values may be sent and summed in bfloat16 or wider, within the bound.
A program may use at most 64 MiB of HBM per device.

```python
import math
import jax
import jax.numpy as jnp
from jax import lax

D = 4096
HEADS = 32
DH = 64
DV = 128
PROP = 16
SEQS = 1
CTX_DEV = 128
TOKENS = 16
POSITIONS = 1024
N_KV = 8
N_TP = 4


def draw_tokens(key, part):
    row_key, column_key, value_key = jax.random.split(key, 3)
    rows = jnp.exp(jax.random.uniform(row_key, (TOKENS, 1), jnp.float32, 0.0, math.log(10.0)))
    rising = jnp.exp(jnp.arange(D, dtype=jnp.float32) * (math.log(3.0) / D))[None, :]
    rough = jnp.exp(jax.random.uniform(column_key, (1, D), jnp.float32, math.log(0.5), math.log(2.0)))
    base = jnp.clip(jax.random.normal(value_key, (TOKENS, D), jnp.float32), -6.0, 6.0)
    return (base * rows * rising * rough / 3.0).astype(jnp.bfloat16)


def draw_key_cache(key, part):
    base_key = jax.random.fold_in(key, 0)
    shape = (SEQS, POSITIONS, HEADS, 2 * DH)
    base = jnp.clip(jax.random.normal(base_key, shape, jnp.float32), -6.0, 6.0)
    return base.astype(jnp.bfloat16)


def draw_parents(key, part):
    raw = jax.random.randint(key, (SEQS, PROP), 0, 1 << 20)
    order = jnp.arange(PROP, dtype=jnp.int32)
    drawn = raw % (order + 1)[None, :] - 1
    last = (order == PROP - 1)[None, :]
    return jnp.where(last, PROP - 2, drawn).astype(jnp.int32)


def steps_of(key, extent, shards, low, high):
    factor_of = 1.0
    for dim, parts in shards:
        heights = jax.random.uniform(jax.random.fold_in(jax.random.fold_in(key, 6), dim), (parts,), jnp.float32, low / len(shards), high / len(shards))
        factor_of = factor_of * jnp.repeat(jnp.exp(heights), extent[dim] // parts).reshape((-1,) + (1,) * (len(extent) - 1 - dim))
    return factor_of


def centred(own_key, extent, width, bound, cuts=(), held_as=jnp.bfloat16):
    level = steps_of(own_key, extent, cuts, -0.22, 0.18) if cuts else 1.0
    array = jax.random.normal(own_key, extent, jnp.float32) * width * level
    return jnp.minimum(jnp.maximum(array, -bound), bound).astype(held_as)


def setup_inputs(seed: int = 0) -> dict:
    key_of = jax.random.split(jax.random.key(seed), 14)
    return {
        "tokens": draw_tokens(jax.random.fold_in(key_of[13], 71), 0),
        "norm_gain": jnp.clip(1.0 + 0.18 * jax.random.normal(key_of[1], (D,), jnp.float32), 0.099609375, 1.8984375).astype(jnp.bfloat16),
        "query_weight": centred(key_of[2], (D, HEADS * 2 * DH), D ** -0.5, 0.09375, ((0, 8), (1, 4))),
        "key_weight": centred(key_of[3], (D, HEADS * 2 * DH), (2.0 * D ** -0.5), 0.5, ((0, 8), (1, 4))),
        "value_weight": centred(key_of[4], (D, HEADS * DV), D ** -0.5, 0.09375, ((0, 8), (1, 4))),
        "out_weight": centred(key_of[5], (HEADS * DV, D), (HEADS * DV) ** -0.5, 0.09375, ((0, 4), (1, 8))),
        "diff_scale": jnp.clip(0.3 + 0.5 * jax.random.uniform(key_of[6], (HEADS,), jnp.float32) ** steps_of(key_of[6], (HEADS,), ((0, 4),), -0.2, 0.2), 0.3, 0.8),
        "head_gain": jnp.clip(1.0 + 0.18 * jax.random.normal(key_of[7], (DV,), jnp.float32), 0.1, 1.9),
        "key_cache": draw_key_cache(jax.random.fold_in(key_of[13], 71), 0),
        "value_cache": centred(key_of[9], (SEQS, POSITIONS, HEADS, DV), 1.0, 6.0, ((1, 8), (2, 4))),
        "cache_filled": jax.random.randint(key_of[10], (SEQS,), POSITIONS // 2, POSITIONS - 2 * PROP + 1).astype(jnp.int32),
        "accepted": jax.random.randint(key_of[11], (SEQS,), 0, PROP + 1).astype(jnp.int32),
        "parents": draw_parents(jax.random.fold_in(key_of[13], 71), 0),
    }


def ancestry(parents):
    links = (parents[:, :, None] == jnp.arange(PROP, dtype=jnp.int32)[None, None, :]).astype(jnp.float32)
    identity = jnp.eye(PROP, dtype=jnp.float32)
    reach = jnp.minimum(identity[None] + links, 1.0)
    for turn in range(PROP.bit_length()):
        reach = jnp.minimum(jnp.einsum('spj,sjk->spk', reach, reach), 1.0)
    return reach > 0.5

def reference(tokens, norm_gain, query_weight, key_weight, value_weight, out_weight, diff_scale, head_gain, key_cache, value_cache, cache_filled, accepted, parents):
    xfloat = tokens.astype(jnp.float32)
    row_scale = lax.rsqrt(lax.optimization_barrier(jnp.mean(xfloat * xfloat, axis=1, keepdims=True)) + 1e-06)
    normed = (xfloat * norm_gain.astype(jnp.float32)).astype(jnp.bfloat16)

    def project(weight):
        return (row_scale * jnp.dot(normed, weight, preferred_element_type=jnp.float32)).astype(jnp.bfloat16)
    queries = project(query_weight).reshape(SEQS, PROP, HEADS, 2, DH)
    new_keys = project(key_weight).reshape(SEQS, PROP, HEADS, 2 * DH)
    new_values = project(value_weight).reshape(SEQS, PROP, HEADS, DV)
    valid_rows = (cache_filled + accepted).astype(jnp.int32)
    reach = ancestry(parents)
    places = jnp.arange(POSITIONS, dtype=jnp.int32).reshape(N_KV, CTX_DEV)
    inv_root = DH ** (-0.5)

    def one_sequence(inputs):
        query, cached_k, cached_v, fresh_k, fresh_v, limit, tree = inputs
        query_f = query.astype(jnp.float32)
        blocks_k = cached_k.reshape(N_KV, CTX_DEV, HEADS, 2, DH).astype(jnp.float32)
        blocks_v = cached_v.reshape(N_KV, CTX_DEV, HEADS, DV).astype(jnp.float32)
        scores = jnp.einsum('phmd,nchmd->nhmpc', query_f, blocks_k) * inv_root
        visible = (places < limit)[:, None, None, None, :]
        local_max = lax.optimization_barrier(jnp.max(jnp.where(visible, scores, -1e+30), axis=-1))
        weights = jnp.where(visible, jnp.exp(scores - local_max[..., None]), 0.0)
        sums = lax.optimization_barrier(jnp.sum(weights, axis=-1))
        weighted = jnp.einsum('nhmpc,nchd->nhmpd', weights.astype(jnp.bfloat16).astype(jnp.float32), blocks_v)
        own_keys = fresh_k.reshape(PROP, HEADS, 2, DH).astype(jnp.float32)
        own_scores = jnp.einsum('phmd,jhmd->hmpj', query_f, own_keys) * inv_root
        own_visible = tree[None, None]
        own_max = lax.optimization_barrier(jnp.max(jnp.where(own_visible, own_scores, -1e+30), axis=-1))
        own_weights = jnp.where(own_visible, jnp.exp(own_scores - own_max[..., None]), 0.0)
        own_sums = lax.optimization_barrier(jnp.sum(own_weights, axis=-1))
        own_weighted = jnp.einsum('hmpj,jhd->hmpd', own_weights.astype(jnp.bfloat16).astype(jnp.float32), fresh_v.astype(jnp.float32))
        highest = jnp.maximum(lax.optimization_barrier(jnp.max(local_max, axis=0)), own_max)
        block_factor = jnp.exp(local_max - highest)
        own_factor = jnp.exp(own_max - highest)
        total = lax.optimization_barrier(jnp.sum(sums * block_factor, axis=0)) + own_sums * own_factor
        values_sum = lax.optimization_barrier(jnp.sum(weighted * block_factor[..., None], axis=0)) + own_weighted * own_factor[..., None]
        return values_sum / total[..., None]
    maps = lax.map(one_sequence, (queries, key_cache, value_cache, new_keys, new_values, valid_rows, reach))
    second_weight = diff_scale.astype(jnp.float32)[None, :, None, None]
    head_out = maps[:, :, 0] - second_weight * maps[:, :, 1]
    head_out = jnp.transpose(head_out, (0, 2, 1, 3)).reshape(TOKENS, HEADS, DV)
    head_out = head_out * lax.rsqrt(lax.optimization_barrier(jnp.mean(head_out * head_out, axis=-1, keepdims=True)) + 1e-05) * head_gain.astype(jnp.float32)
    flat = head_out.astype(jnp.bfloat16).reshape(TOKENS, N_TP, HEADS // N_TP * DV)
    groups = out_weight.reshape(N_TP, HEADS // N_TP * DV, D)
    mixed = jnp.zeros((TOKENS, D), jnp.float32)
    for group in range(N_TP):
        mixed = mixed + jnp.dot(flat[:, group], groups[group], preferred_element_type=jnp.float32).astype(jnp.bfloat16).astype(jnp.float32)

    def write(cache, fresh, start):
        zero = jnp.zeros((), jnp.int32)
        return lax.dynamic_update_slice(cache, fresh.astype(cache.dtype), (start.astype(jnp.int32), zero, zero))
    key_cache_new = jax.vmap(write)(key_cache, new_keys, valid_rows)
    value_cache_new = jax.vmap(write)(value_cache, new_values, valid_rows)
    return (mixed.astype(jnp.bfloat16), key_cache_new, value_cache_new)
```

```python
import functools

import jax
import jax.numpy as jnp
from jax import lax
from jax.experimental import pallas as pl
from jax.experimental.pallas import tpu as pltpu
from jax.sharding import PartitionSpec as P

D = 4096
DH = 64
DV = 128


def joined(value, axis, join):
    pieces = jax.tree.map(lambda part: lax.all_gather(part, axis), value)
    head = jax.tree.map(lambda part: part[0], pieces)
    tail = jax.tree.map(lambda part: part[1:], pieces)
    so_far, _ = lax.scan(lambda so_far, share: (join(so_far, share), None), head, tail)
    return so_far


def ancestry(parents):
    count = parents.shape[1]
    links = (parents[:, :, None] == jnp.arange(count, dtype=jnp.int32)[None, None, :]).astype(
        jnp.float32
    )
    identity = jnp.eye(count, dtype=jnp.float32)
    reach = jnp.minimum(identity[None] + links, 1.0)
    for turn in range(count.bit_length()):
        reach = jnp.minimum(jnp.einsum("spj,sjk->spk", reach, reach), 1.0)
    return reach > 0.5


def combine(earlier, later):
    highest = jnp.maximum(earlier[0], later[0])
    factor_one = jnp.exp(earlier[0] - highest)
    factor_two = jnp.exp(later[0] - highest)
    total = earlier[1] * factor_one + later[1] * factor_two
    values_sum = earlier[2] * factor_one[..., None] + later[2] * factor_two[..., None]
    return (highest, total, values_sum)


def head_norm(head_out, head_gain):
    return (
        head_out
        * lax.rsqrt(jnp.mean(head_out * head_out, axis=-1, keepdims=True) + 1e-05)
        * head_gain
    )


def shards(
    tokens,
    norm_gain,
    query_weight,
    key_weight,
    value_weight,
    out_weight,
    diff_scale,
    head_gain,
    key_cache,
    value_cache,
    cache_filled,
    accepted,
    parents,
):
    seq_count = key_cache.shape[0]
    span = key_cache.shape[1]
    heads_here = key_cache.shape[2]
    proposals = tokens.shape[0] // seq_count
    inv_root = DH ** (-0.5)
    xfloat = tokens.astype(jnp.float32)
    squares = jnp.sum(xfloat * xfloat, axis=1)
    normed = (xfloat * norm_gain.astype(jnp.float32)).astype(jnp.bfloat16)
    partial_value = jnp.concatenate(
        [
            jnp.dot(normed, query_weight, preferred_element_type=jnp.float32),
            jnp.dot(normed, key_weight, preferred_element_type=jnp.float32),
            jnp.dot(normed, value_weight, preferred_element_type=jnp.float32),
        ],
        axis=1,
    )
    totals, square_sum = lax.psum((partial_value, squares), "kv")
    row_scale = lax.rsqrt(square_sum / D + 1e-06)
    projected = (totals * row_scale[:, None]).astype(jnp.bfloat16)
    q_width = heads_here * 2 * DH
    queries = projected[:, :q_width].reshape(seq_count, proposals, heads_here, 2, DH)
    fresh_k = projected[:, q_width : 2 * q_width].reshape(seq_count, proposals, heads_here * 2 * DH)
    fresh_v = projected[:, 2 * q_width :].reshape(seq_count, proposals, heads_here * DV)
    cached_k = key_cache.reshape(seq_count, span, heads_here, 2, DH)
    scores = (
        jnp.einsum("sphmd,schmd->shmpc", queries, cached_k, preferred_element_type=jnp.float32)
        * inv_root
    )
    places = lax.axis_index("kv") * span + jnp.arange(span, dtype=jnp.int32)
    valid_rows = cache_filled + accepted
    visible = (places[None, :] < valid_rows[:, None])[:, None, None, None, :]
    local_max = jnp.max(jnp.where(visible, scores, -1e30), axis=-1)
    weights = jnp.where(visible, jnp.exp(scores - local_max[..., None]), 0.0)
    sums = jnp.sum(weights, axis=-1)
    weighted = jnp.einsum(
        "shmpc,schd->shmpd",
        weights.astype(jnp.bfloat16),
        value_cache,
        preferred_element_type=jnp.float32,
    )
    reach = ancestry(parents)
    own_keys = fresh_k.reshape(seq_count, proposals, heads_here, 2, DH)
    own_scores = (
        jnp.einsum("sphmd,sjhmd->shmpj", queries, own_keys, preferred_element_type=jnp.float32)
        * inv_root
    )
    own_visible = reach[:, None, None]
    own_max = jnp.max(jnp.where(own_visible, own_scores, -1e30), axis=-1)
    own_weights = jnp.where(own_visible, jnp.exp(own_scores - own_max[..., None]), 0.0)
    own_sums = jnp.sum(own_weights, axis=-1)
    own_values = fresh_v.reshape(seq_count, proposals, heads_here, DV)
    own_weighted = jnp.einsum(
        "shmpj,sjhd->shmpd",
        own_weights.astype(jnp.bfloat16),
        own_values,
        preferred_element_type=jnp.float32,
    )
    highest, total, values_sum = combine(
        joined((local_max, sums, weighted), "kv", combine), (own_max, own_sums, own_weighted)
    )
    maps = values_sum / total[..., None]
    second_weight = diff_scale[None, :, None, None]
    head_out = maps[:, :, 0] - second_weight * maps[:, :, 1]
    head_out = head_norm(jnp.transpose(head_out, (0, 2, 1, 3)), head_gain)
    flat = head_out.astype(jnp.bfloat16).reshape(seq_count * proposals, heads_here * DV)
    partial_out = jnp.dot(flat, out_weight, preferred_element_type=jnp.float32)
    mixed = lax.psum(partial_out.astype(jnp.bfloat16), "tp")
    relative = places[None, :] - valid_rows[:, None]
    one_hot = (
        relative[:, :, None] == jnp.arange(proposals, dtype=jnp.int32)[None, None, :]
    ).astype(jnp.bfloat16)
    inside = ((relative >= 0) & (relative < proposals))[:, :, None]
    placed_k = jnp.einsum(
        "scj,sjx->scx", one_hot, fresh_k, preferred_element_type=jnp.float32
    ).astype(jnp.bfloat16)
    placed_v = jnp.einsum(
        "scj,sjx->scx", one_hot, fresh_v, preferred_element_type=jnp.float32
    ).astype(jnp.bfloat16)
    key_out = jnp.where(
        inside, placed_k, key_cache.reshape(seq_count, span, heads_here * 2 * DH)
    ).reshape(key_cache.shape)
    value_out = jnp.where(
        inside, placed_v, value_cache.reshape(seq_count, span, heads_here * DV)
    ).reshape(value_cache.shape)
    return (mixed, key_out, value_out)


MESH = pl.DeviceIdType.MESH
BF = jnp.bfloat16
F32 = jnp.float32
PART = jnp.float32
UTYPE = jnp.bfloat16
VMEM_BYTES = 67043328


def dot(a, b):
    return jnp.dot(a, b, preferred_element_type=F32)


def iota(shape, dim):
    return lax.broadcasted_iota(jnp.int32, shape, dim)


def kernel(
    n,
    n_tp,
    heads,
    tok_hbm,
    gain_hbm,
    hgain_hbm,
    wq_hbm,
    wk_hbm,
    wv_hbm,
    wo_hbm,
    kc_hbm,
    vc_hbm,
    scale_hbm,
    filled_hbm,
    accepted_hbm,
    parents_hbm,
    mixed_ref,
    ko,
    vo,
    tok_ref,
    gain_ref,
    hgain_ref,
    wq,
    wk,
    wv,
    wo,
    kc,
    vc,
    kf,
    vf,
    kh,
    vh,
    sq_send,
    sq_recv,
    q_send,
    q_recv,
    kv_send,
    kv_recv,
    qg_send,
    qg_recv,
    kvg_send,
    kvg_recv,
    u_send,
    u_recv,
    ms_send,
    ms_recv,
    hg_send,
    hg_recv,
    m_send,
    m_recv,
    scale_ref,
    filled_ref,
    accepted_ref,
    parents_ref,
    local_sem,
    send_sem,
    recv_sem,
    tsend_sem,
    trecv_sem,
):
    me = lax.axis_index("kv")
    tp = lax.axis_index("tp")
    rows = tok_ref.shape[0]
    pair = 2 * rows
    loads = []
    for i, (src, dst) in enumerate(
        (
            (tok_hbm, tok_ref),
            (gain_hbm, gain_ref),
            (wq_hbm, wq),
            (wk_hbm, wk),
            (wv_hbm, wv),
            (kc_hbm, kc),
            (vc_hbm, vc),
            (hgain_hbm, hgain_ref),
            (wo_hbm, wo),
            (scale_hbm, scale_ref),
            (filled_hbm, filled_ref),
            (accepted_hbm, accepted_ref),
            (parents_hbm, parents_ref),
        )
    ):
        load = pltpu.make_async_copy(src, dst, local_sem.at[i])
        load.start()
        loads.append(load)
    peers = [lax.rem(me + off, n) for off in range(1, n)]
    tpeers = [lax.rem(tp + off, n_tp) for off in range(1, n_tp)]
    barrier = pltpu.get_barrier_semaphore()
    for peer in peers:
        pl.semaphore_signal(barrier, inc=1, device_id={"kv": peer}, device_id_type=MESH)
    for peer in tpeers:
        pl.semaphore_signal(barrier, inc=1, device_id={"tp": peer}, device_id_type=MESH)

    started = []

    def spread(phase, pick, recv):
        for peer in peers:
            copy = pltpu.make_async_remote_copy(
                src_ref=pick(peer),
                dst_ref=recv.at[me],
                send_sem=send_sem.at[phase, peer],
                recv_sem=recv_sem.at[phase, me],
                device_id={"kv": peer},
                device_id_type=MESH,
            )
            copy.start()
            started.append(copy)

    def arrive(phase, recv):
        for peer in peers:
            pltpu.make_async_remote_copy(
                src_ref=recv.at[peer],
                dst_ref=recv.at[peer],
                send_sem=send_sem.at[phase, peer],
                recv_sem=recv_sem.at[phase, peer],
                device_id={"kv": peer},
                device_id_type=MESH,
            ).wait_recv()

    loads[0].wait()
    for i in range(9, 13):
        loads[i].wait()
    loads[1].wait()
    xfloat = tok_ref[...].astype(F32)
    squares = jnp.sum(xfloat * xfloat, axis=1, keepdims=True)
    sq_send[...] = jnp.broadcast_to(squares, sq_send.shape)
    gain = gain_ref[...].astype(F32)
    gain = jnp.concatenate([gain[i : i + 1] for i in range(gain.shape[0])], axis=1)
    normed = (xfloat * gain).astype(BF)

    links = jnp.zeros((rows, rows), F32)
    sub, lane = iota((rows, rows), 0), iota((rows, rows), 1)
    for p in range(rows):
        links = jnp.where((sub == p) & (lane == parents_ref[0, p]), 1.0, links)
    reach = jnp.where(sub == lane, 1.0, links)
    for turn in range((rows - 1).bit_length()):
        reach = jnp.minimum(dot(reach.astype(BF), reach.astype(BF)), 1.0)

    loads[2].wait()
    part = dot(normed, wq[...])
    for h in range(heads):
        q_send[h] = part[:, h * DV : (h + 1) * DV].astype(PART)
    pl.semaphore_wait(barrier, (n - 1) + (n_tp - 1))
    spread(0, lambda peer: sq_send, sq_recv)
    spread(1, lambda peer: q_send.at[peer], q_recv)
    loads[3].wait()
    part = dot(normed, wk[...])
    for h in range(heads):
        kv_send[h, :rows] = part[:, h * DV : (h + 1) * DV].astype(PART)
    loads[4].wait()
    part = dot(normed, wv[...])
    for h in range(heads):
        kv_send[h, rows:] = part[:, h * DV : (h + 1) * DV].astype(PART)
    spread(2, lambda peer: kv_send.at[peer], kv_recv)

    count = kc.shape[0]
    span = count // heads
    loads[5].wait()
    loads[6].wait()
    loads[7].wait()
    for cache, wide, by_head in ((kc, kf, kh), (vc, vf, vh)):
        wide[...] = cache[...].astype(F32)
        for h in range(heads):
            by_head[h] = wide[pl.ds(h, span, stride=heads), :].astype(BF)

    sq_recv[me] = sq_send[...]
    q_recv[me] = q_send[me]
    arrive(0, sq_recv)
    total = sq_recv[0]
    for i in range(1, n):
        total = total + sq_recv[i]
    row_scale = lax.rsqrt(total / (n * tok_ref.shape[1]) + 1e-06)
    arrive(1, q_recv)
    q_sum = q_recv[0].astype(F32)
    for i in range(1, n):
        q_sum = q_sum + q_recv[i].astype(F32)
    query = (q_sum * row_scale).astype(BF)
    qg_send[...] = query
    spread(3, lambda peer: qg_send, qg_recv)
    qg_recv[me] = query

    kv_recv[me] = kv_send[me]
    arrive(2, kv_recv)
    kv_sum = kv_recv[0].astype(F32)
    for i in range(1, n):
        kv_sum = kv_sum + kv_recv[i].astype(F32)
    fresh_k = (kv_sum[:rows] * row_scale).astype(BF)
    fresh_v = (kv_sum[rows:] * row_scale).astype(BF)
    kvg_send[:rows] = fresh_k
    kvg_send[rows:] = fresh_v
    spread(4, lambda peer: kvg_send, kvg_recv)
    kvg_recv[me, :rows] = fresh_k
    kvg_recv[me, rows:] = fresh_v

    inv_root = DH ** (-0.5)
    first_map = iota((rows, DV), 1) < DH

    def two_maps(query):
        scaled = query.astype(F32) * inv_root
        one = jnp.where(first_map, scaled, 0.0).astype(BF)
        two = jnp.where(first_map, 0.0, scaled).astype(BF)
        return jnp.concatenate([one, two], axis=0)

    def scored(q, k):
        return lax.dot_general(q, k, (((1,), (1,)), ((), ())), preferred_element_type=F32)

    own = scored(two_maps(query), fresh_k)
    seen = jnp.concatenate([reach, reach], axis=0) > 0.5
    own = jnp.where(seen, own, -1e30)
    own_max = jnp.max(own, axis=1, keepdims=True)
    own_weights = jnp.exp(own - own_max)
    own_sums = jnp.sum(own_weights, axis=1, keepdims=True)
    own_weighted = dot(own_weights.astype(BF), fresh_v)
    eye = iota((pair, DV), 0) == iota((pair, DV), 1)

    def as_row(column):
        return jnp.sum(jnp.where(eye, column, 0.0), axis=0, keepdims=True)

    def as_column(row):
        return jnp.sum(jnp.where(eye, row, 0.0), axis=1, keepdims=True)

    own_max_row = as_row(own_max)
    own_sums_row = as_row(own_sums)

    shift = heads.bit_length() - 1
    valid = filled_ref[0] + accepted_ref[0]
    visible = me * span + iota((1, span), 1) < valid
    arrive(3, qg_recv)
    scores = jnp.concatenate([scored(two_maps(qg_recv[h]), kh[h]) for h in range(heads)], axis=0)
    scores = jnp.where(visible, scores, -1e30)
    highest = jnp.maximum(jnp.max(scores, axis=1, keepdims=True), -1e29)
    weights = jnp.exp(scores - highest)
    sums = jnp.sum(weights, axis=1, keepdims=True)
    weights = weights.astype(BF)
    top = iota((8, DV), 0) == 0
    for h in range(heads):
        part_of = slice(h * pair, (h + 1) * pair)
        u_send[h] = dot(weights[part_of], vh[h]).astype(UTYPE)
        ms_send[h] = jnp.where(top, as_row(highest[part_of]), as_row(sums[part_of]))
    spread(5, lambda peer: ms_send.at[peer], ms_recv)
    spread(6, lambda peer: u_send.at[peer], u_recv)
    ms_recv[me] = ms_send[me]
    u_recv[me] = u_send[me]

    arrive(4, kvg_recv)
    line = iota((count, DV), 0)
    relative = me * span + (line >> shift) - valid
    inside = (relative >= 0) & (relative < rows)
    target = (line & (heads - 1)) * rows + relative
    one_hot = jnp.where(inside & (target == iota((count, DV), 1)), 1.0, 0.0).astype(BF)
    all_k = jnp.concatenate([kvg_recv[h, :rows] for h in range(heads)], axis=0)
    all_v = jnp.concatenate([kvg_recv[h, rows:] for h in range(heads)], axis=0)
    ko[...] = jnp.where(inside, dot(one_hot, all_k), kc[...].astype(F32)).astype(BF)
    vo[...] = jnp.where(inside, dot(one_hot, all_v), vc[...].astype(F32)).astype(BF)
    arrive(5, ms_recv)
    peak = own_max_row
    for i in range(n):
        peak = jnp.maximum(peak, ms_recv[i, 0:1])
    factors = []
    own_factor = jnp.exp(own_max_row - peak)
    whole = own_sums_row * own_factor
    for i in range(n):
        factor = jnp.exp(ms_recv[i, 0:1] - peak)
        whole = whole + ms_recv[i, 1:2] * factor
        factors.append(factor)
    merged = own_weighted * as_column(own_factor / whole)
    shares = [as_column(factor / whole) for factor in factors]
    arrive(6, u_recv)
    for i in range(n):
        merged = merged + u_recv[i].astype(F32) * shares[i]
    head_out = merged[:rows] - scale_ref[me] * merged[rows:]
    spreadness = jnp.mean(head_out * head_out, axis=1, keepdims=True)
    head_out = (head_out * lax.rsqrt(spreadness + 1e-05) * hgain_ref[...]).astype(BF)
    hg_send[...] = head_out
    spread(7, lambda peer: hg_send, hg_recv)
    hg_recv[me] = head_out
    loads[8].wait()
    arrive(7, hg_recv)
    flat = jnp.concatenate([hg_recv[h] for h in range(heads)], axis=1)
    out = dot(flat, wo[...]).astype(BF)
    m_send[...] = out
    tcopies = []
    for peer in tpeers:
        copy = pltpu.make_async_remote_copy(
            src_ref=m_send,
            dst_ref=m_recv.at[tp],
            send_sem=tsend_sem.at[peer],
            recv_sem=trecv_sem.at[tp],
            device_id={"tp": peer},
            device_id_type=MESH,
        )
        copy.start()
        tcopies.append(copy)
    m_recv[tp] = out
    for copy in started:
        copy.wait_send()
    for peer in tpeers:
        pltpu.make_async_remote_copy(
            src_ref=m_recv.at[peer],
            dst_ref=m_recv.at[peer],
            send_sem=tsend_sem.at[peer],
            recv_sem=trecv_sem.at[peer],
            device_id={"tp": peer},
            device_id_type=MESH,
        ).wait_recv()
    mixed = m_recv[0].astype(F32)
    for i in range(1, n_tp):
        mixed = mixed + m_recv[i].astype(F32)
    mixed_ref[...] = mixed.astype(BF)
    for copy in tcopies:
        copy.wait_send()


def deliver(mixed, key, value, mixed_hbm, key_hbm, value_hbm, sem):
    copies = [
        pltpu.make_async_copy(src, dst, sem.at[i])
        for i, (src, dst) in enumerate(((key, key_hbm), (value, value_hbm), (mixed, mixed_hbm)))
    ]
    for copy in copies:
        copy.start()
    for copy in copies:
        copy.wait()


def fused(
    n,
    n_tp,
    tokens,
    norm_gain,
    query_weight,
    key_weight,
    value_weight,
    out_weight,
    diff_scale,
    head_gain,
    key_cache,
    value_cache,
    cache_filled,
    accepted,
    parents,
):
    rows, features = tokens.shape
    heads = key_cache.shape[2]
    count = key_cache.shape[1] * heads
    width = out_weight.shape[1]
    vmem = pl.BlockSpec(memory_space=pltpu.VMEM)
    smem = pl.BlockSpec(memory_space=pltpu.SMEM)
    hbm = pl.BlockSpec(memory_space=pltpu.HBM)
    cache_shape = pltpu.VMEM((count, DV), BF)
    kept = 2 * (rows * width + 2 * count * DV) + (1 << 14)
    mixed, key_out, value_out = pl.pallas_call(
        functools.partial(kernel, n, n_tp, heads),
        out_shape=(pltpu.VMEM((rows, width), BF), cache_shape, cache_shape),
        in_specs=[hbm] * 13,
        out_specs=(vmem, vmem, vmem),
        scratch_shapes=[
            pltpu.VMEM(tokens.shape, BF),
            pltpu.VMEM((features // DV, DV), BF),
            pltpu.VMEM((1, DV), F32),
            pltpu.VMEM(query_weight.shape, BF),
            pltpu.VMEM(key_weight.shape, BF),
            pltpu.VMEM(value_weight.shape, BF),
            pltpu.VMEM(out_weight.shape, BF),
            pltpu.VMEM((count, DV), BF),
            pltpu.VMEM((count, DV), BF),
            pltpu.VMEM((count, DV), F32),
            pltpu.VMEM((count, DV), F32),
            pltpu.VMEM((heads, count // heads, DV), BF),
            pltpu.VMEM((heads, count // heads, DV), BF),
            pltpu.VMEM((rows, DV), F32),
            pltpu.VMEM((n, rows, DV), F32),
            pltpu.VMEM((heads, rows, DV), PART),
            pltpu.VMEM((n, rows, DV), PART),
            pltpu.VMEM((heads, 2 * rows, DV), PART),
            pltpu.VMEM((n, 2 * rows, DV), PART),
            pltpu.VMEM((rows, DV), BF),
            pltpu.VMEM((n, rows, DV), BF),
            pltpu.VMEM((2 * rows, DV), BF),
            pltpu.VMEM((n, 2 * rows, DV), BF),
            pltpu.VMEM((heads, 2 * rows, DV), UTYPE),
            pltpu.VMEM((n, 2 * rows, DV), UTYPE),
            pltpu.VMEM((heads, 8, DV), F32),
            pltpu.VMEM((n, 8, DV), F32),
            pltpu.VMEM((rows, DV), BF),
            pltpu.VMEM((n, rows, DV), BF),
            pltpu.VMEM((rows, width), BF),
            pltpu.VMEM((n_tp, rows, width), BF),
            pltpu.SMEM((heads,), F32),
            pltpu.SMEM((1,), jnp.int32),
            pltpu.SMEM((1,), jnp.int32),
            pltpu.SMEM(parents.shape, jnp.int32),
            pltpu.SemaphoreType.DMA((13,)),
            pltpu.SemaphoreType.DMA((8, n)),
            pltpu.SemaphoreType.DMA((8, n)),
            pltpu.SemaphoreType.DMA((n_tp,)),
            pltpu.SemaphoreType.DMA((n_tp,)),
        ],
        compiler_params=pltpu.CompilerParams(collective_id=0, has_side_effects=True, vmem_limit_bytes=VMEM_BYTES - kept),
    )(
        tokens,
        norm_gain.reshape(features // DV, DV),
        head_gain.reshape(1, DV),
        query_weight,
        key_weight,
        value_weight,
        out_weight,
        key_cache.reshape(count, DV),
        value_cache.reshape(count, DV),
        diff_scale,
        cache_filled,
        accepted,
        parents,
    )
    flat = [jax.ShapeDtypeStruct(out.shape, out.dtype) for out in (mixed, key_out, value_out)]
    mixed, key_out, value_out = pl.pallas_call(
        deliver,
        out_shape=flat,
        in_specs=[vmem] * 3,
        out_specs=[hbm] * 3,
        scratch_shapes=[pltpu.SemaphoreType.DMA((3,))],
        compiler_params=pltpu.CompilerParams(vmem_limit_bytes=4 << 20),
    )(mixed, key_out, value_out)
    return mixed, key_out.reshape(key_cache.shape), value_out.reshape(value_cache.shape)


def body(n, n_tp, *args):
    tokens, key_cache = args[0], args[8]
    seqs, heads = key_cache.shape[0], key_cache.shape[2]
    rows = tokens.shape[0]
    if seqs == 1 and heads == n and heads & (heads - 1) == 0 and rows % 16 == 0 and 2 * rows <= DV and tokens.shape[1] % DV == 0:
        return fused(n, n_tp, *args)
    return shards(*args)


def solution(mesh):
    in_specs = (
        P(None, "kv"),
        P("kv"),
        P("kv", "tp"),
        P("kv", "tp"),
        P("kv", "tp"),
        P("tp", "kv"),
        P("tp"),
        P(),
        P(None, "kv", "tp", None),
        P(None, "kv", "tp", None),
        P(),
        P(),
        P(),
    )
    out_specs = (P(None, "kv"), P(None, "kv", "tp", None), P(None, "kv", "tp", None))
    return jax.shard_map(
        functools.partial(body, mesh.shape["kv"], mesh.shape["tp"]), mesh=mesh, in_specs=in_specs, out_specs=out_specs, check_vma=False)
```
